32 devices in a mesh: sp: 8 (over z, x), tp: 4 (over y, core).
Axes of the slice: x: 2, y: 2, z: 4, core: 2. Of those that a mesh axis runs over, the one named last changes fastest.
Arguments:
- stream: bfloat16 [2048, 2048], P(('sp', 'tp')), may hold values from -6 to 6
- query_a: bfloat16 [2048, 384], P('sp', 'tp'), may hold values from -400 to 400
- query_b: bfloat16 [2048, 640], P('sp', 'tp'), may hold values from -400 to 400
- latent: bfloat16 [2048, 256], P('sp'), may hold values from -6 to 6
- rotary_key: bfloat16 [2048, 32], P('sp'), may hold values from -6 to 6
- latent_gain: float32 [256], replicated, may hold values from 0.1 to 1.9
- key_gain_a: float32 [96], replicated, may hold values from 0.1 to 1.9
- key_gain_b: float32 [160], replicated, may hold values from 0.1 to 1.9
- w_key_a: bfloat16 [256, 256], P(None, 'tp'), may hold values from -0.375 to 0.375
- w_value_a: bfloat16 [256, 256], P(None, 'tp'), may hold values from -0.375 to 0.375
- w_key_b: bfloat16 [256, 512], P(None, 'tp'), may hold values from -0.375 to 0.375
- w_value_b: bfloat16 [256, 512], P(None, 'tp'), may hold values from -0.375 to 0.375
- w_out_a: bfloat16 [256, 2048], P('tp'), may hold values from -0.21875 to 0.21875
- w_out_b: bfloat16 [512, 2048], P('tp'), may hold values from -0.21875 to 0.21875
- norm_gain: float32 [2048], replicated, may hold values from 0.1 to 1.9
- w_up: bfloat16 [2048, 4096], P('sp', 'tp'), may hold values from -0.125 to 0.125
- w_down: bfloat16 [4096, 2048], P('tp', 'sp'), may hold values from -0.09375 to 0.09375
Outputs:
- result: bfloat16 [2048, 2048], P(('sp', 'tp'))
The draws below stay inside these ranges and needn't reach their ends.
All inputs are finite; a program needn't handle non-finite values.
Results may differ from the reference program's by a relative error of at most 0.018.
The reference program's roundings to bfloat16 on the way count: a program that leaves them out, or rounds other values in their place, can miss the bound.
Values may be sent and summed in bfloat16 or wider, within the bound.
No kernel may reach another device: no remote copies, remote signals or barrier semaphores. Data moves between devices by JAX's collectives and lax.ppermute only.
A program may use at most 128 MiB of HBM per device.

```python
import math
import jax
import jax.numpy as jnp
from jax import lax

D = 2048
HEADS_A = 4
HEADS_B = 4
NOPE_A = 64
V_A = 64
NOPE_B = 128
V_B = 128
ROPE = 32
KV_RANK = 256
FF = 4096
TOKENS = 2048


def scaled_rows(key, count, width):
    base_key = jax.random.fold_in(key, 0)
    base = jax.random.normal(base_key, (count, width), jnp.float32)
    factor = 2.5 * jnp.ones((count, 1), jnp.float32)
    return jnp.clip(base * factor, -400.0, 400.0)


def draw_query_a(key, part):
    return scaled_rows(jax.random.fold_in(key, 11), TOKENS, HEADS_A * (NOPE_A + ROPE)).astype(jnp.bfloat16)


def draw_query_b(key, part):
    return scaled_rows(jax.random.fold_in(key, 23), TOKENS, HEADS_B * (NOPE_B + ROPE)).astype(jnp.bfloat16)


def block_scale(stream_key, shape, shards, smallest, largest):
    level = 1.0
    for position, blocks in shards:
        heights = jax.random.uniform(jax.random.fold_in(jax.random.fold_in(stream_key, 6), position), (blocks,), jnp.float32, smallest / len(shards), largest / len(shards))
        level = level * jnp.repeat(jnp.exp(heights), shape[position] // blocks).reshape((-1,) + (1,) * (len(shape) - 1 - position))
    return level


def scatter_about(own_key, shape, scale, reach, cuts=(), kind=jnp.bfloat16):
    array = scale * jax.random.normal(own_key, shape, jnp.float32)
    if cuts:
        array = array * block_scale(own_key, shape, cuts, -0.22, 0.18)
    return jnp.clip(array, -reach, reach).astype(kind)


def setup_inputs(seed: int = 0) -> dict:
    splits = jax.random.split(jax.random.key(seed), 18)
    stream = scatter_about(splits[0], (TOKENS, D), 0.4, 6.0, ((0, 32),))
    query_a = draw_query_a(jax.random.fold_in(splits[17], 71), 0)
    query_b = draw_query_b(jax.random.fold_in(splits[17], 71), 0)
    latent = scatter_about(splits[3], (TOKENS, KV_RANK), 1.0, 6.0, ((0, 8),))
    rotary_key = scatter_about(splits[4], (TOKENS, ROPE), 1.0, 6.0, ((0, 8),))
    latent_gain = jnp.clip(1.0 + 0.18 * jax.random.normal(splits[5], (KV_RANK,), jnp.float32), 0.1, 1.9)
    key_gain_a = jnp.clip(1.0 + 0.18 * jax.random.normal(splits[6], (NOPE_A + ROPE,), jnp.float32), 0.1, 1.9)
    key_gain_b = jnp.clip(1.0 + 0.18 * jax.random.normal(splits[7], (NOPE_B + ROPE,), jnp.float32), 0.1, 1.9)
    w_key_a = scatter_about(splits[8], (KV_RANK, HEADS_A * NOPE_A), KV_RANK ** -0.5, 0.375, ((1, 4),))
    w_value_a = scatter_about(splits[9], (KV_RANK, HEADS_A * V_A), KV_RANK ** -0.5, 0.375, ((1, 4),))
    w_key_b = scatter_about(splits[10], (KV_RANK, HEADS_B * NOPE_B), KV_RANK ** -0.5, 0.375, ((1, 4),))
    w_value_b = scatter_about(splits[11], (KV_RANK, HEADS_B * V_B), KV_RANK ** -0.5, 0.375, ((1, 4),))
    w_out_a = scatter_about(splits[12], (HEADS_A * V_A, D), (HEADS_A * V_A + HEADS_B * V_B) ** -0.5, 0.21875, ((0, 4),))
    w_out_b = scatter_about(splits[13], (HEADS_B * V_B, D), (HEADS_A * V_A + HEADS_B * V_B) ** -0.5, 0.21875, ((0, 4),))
    norm_gain = jnp.clip(1.0 + 0.18 * jax.random.normal(splits[14], (D,), jnp.float32), 0.1, 1.9)
    w_up = scatter_about(splits[15], (D, FF), D ** -0.5, 0.125, ((0, 8), (1, 4)))
    w_down = scatter_about(splits[16], (FF, D), FF ** -0.5, 0.09375, ((0, 4), (1, 8)))
    return {"stream": stream, "query_a": query_a, "query_b": query_b, "latent": latent, "rotary_key": rotary_key, "latent_gain": latent_gain, "key_gain_a": key_gain_a, "key_gain_b": key_gain_b, "w_key_a": w_key_a, "w_value_a": w_value_a, "w_key_b": w_key_b, "w_value_b": w_value_b, "w_out_a": w_out_a, "w_out_b": w_out_b, "norm_gain": norm_gain, "w_up": w_up, "w_down": w_down}


EPSILON = 1e-06
THETA = 10000.0

def rms_scale(values, gain):
    wide = values.astype(jnp.float32)
    return wide * lax.rsqrt(lax.optimization_barrier(jnp.mean(wide * wide, axis=-1, keepdims=True)) + EPSILON) * gain.astype(jnp.float32)

def rotate(tail, positions):
    half = tail.shape[-1] // 2
    freqs = THETA ** (-jnp.arange(half, dtype=jnp.float32) / half)
    angle = positions[:, None, None] * freqs
    cosine = jnp.cos(angle)
    sine = jnp.sin(angle)
    first = tail[..., :half]
    second = tail[..., half:]
    return jnp.concatenate([first * cosine - second * sine, second * cosine + first * sine], axis=-1)

def make_keys(normed, rotary_key, w_key, w_value, key_gain, nope, positions):
    count = normed.shape[0]
    heads = w_key.shape[1] // nope
    head_nope = jnp.dot(normed, w_key, preferred_element_type=jnp.float32).astype(jnp.bfloat16)
    head_nope = head_nope.reshape(count, heads, nope)
    values = jnp.dot(normed, w_value, preferred_element_type=jnp.float32).astype(jnp.bfloat16)
    shared = jnp.broadcast_to(rotary_key[:, None, :], (count, heads, rotary_key.shape[1]))
    joined = rms_scale(jnp.concatenate([head_nope, shared], axis=-1), key_gain)
    turned = rotate(joined[..., nope:], positions)
    keys_out = jnp.concatenate([joined[..., :nope], turned], axis=-1).astype(jnp.bfloat16)
    return (keys_out.reshape(count, -1), values)

def attention(queries, keys_in, values_in, depth):
    total_rows = keys_in.shape[0]
    heads = keys_in.shape[1] // depth
    key_view = keys_in.astype(jnp.float32).reshape(total_rows, heads, depth)
    value_view = values_in.astype(jnp.float32).reshape(total_rows, heads, -1)
    block = math.gcd(queries.shape[0], 512)
    blocks = queries.astype(jnp.float32).reshape(-1, block, heads, depth)

    def one_block(block_queries):
        scores = jnp.einsum('qhd,khd->qhk', block_queries, key_view) * depth ** (-0.5)
        peak = lax.optimization_barrier(jnp.max(scores, axis=-1))
        shifted = jnp.exp(scores - peak[..., None])
        totals = lax.optimization_barrier(jnp.sum(shifted, axis=-1))
        weights = lax.optimization_barrier(shifted.astype(jnp.bfloat16)).astype(jnp.float32)
        weighted = jnp.einsum('qhk,khd->qhd', weights, value_view)
        return (weighted / totals[..., None]).astype(jnp.bfloat16).reshape(block, -1)
    return lax.map(one_block, blocks).reshape(queries.shape[0], -1)

def reference(stream, query_a, query_b, latent, rotary_key, latent_gain, key_gain_a, key_gain_b, w_key_a, w_value_a, w_key_b, w_value_b, w_out_a, w_out_b, norm_gain, w_up, w_down):
    positions = jnp.arange(TOKENS).astype(jnp.float32)
    normed_latent = rms_scale(latent, latent_gain).astype(jnp.bfloat16)
    key_a, value_a = make_keys(normed_latent, rotary_key, w_key_a, w_value_a, key_gain_a, NOPE_A, positions)
    key_b, value_b = make_keys(normed_latent, rotary_key, w_key_b, w_value_b, key_gain_b, NOPE_B, positions)
    attended_a = attention(query_a, key_a, value_a, NOPE_A + ROPE)
    attended_b = attention(query_b, key_b, value_b, NOPE_B + ROPE)
    mixed = jnp.dot(attended_a, w_out_a, preferred_element_type=jnp.float32) + jnp.dot(attended_b, w_out_b, preferred_element_type=jnp.float32)
    residual = (stream.astype(jnp.float32) + mixed).astype(jnp.bfloat16)
    normed = rms_scale(residual, norm_gain).astype(jnp.bfloat16)
    activated = jnp.square(jax.nn.relu(jnp.dot(normed, w_up, preferred_element_type=jnp.float32))).astype(jnp.bfloat16)
    summed = jnp.dot(activated, w_down, preferred_element_type=jnp.float32)
    return (residual.astype(jnp.float32) + summed).astype(jnp.bfloat16)
```

```python
import jax
import jax.numpy as jnp
from jax import lax
from jax.sharding import PartitionSpec as P

NOPE_A = 64
V_A = 64
NOPE_B = 128
V_B = 128
ROPE = 32


EPSILON = 1e-06
THETA = 10000.0


def rms_scale(values, gain):
    wide = values.astype(jnp.float32)
    return wide * lax.rsqrt(jnp.mean(wide * wide, axis=-1, keepdims=True) + EPSILON) * gain


def dot32(a, b):
    return jnp.dot(a, b, preferred_element_type=jnp.float32)


def pick(array, index, axis):
    return lax.dynamic_index_in_dim(array, index, axis, keepdims=False)


def xor_perm(size, bit):
    return [(i, i ^ bit) for i in range(size)]


def ring_order(size):
    return list(range(0, size, 2)) + list(range(size - 1, 0, -2))


def gather_xor(block, axis, size):
    parts = [(0, block)]
    bit = size // 2
    while bit:
        sent = jnp.stack([p for _, p in parts]) if len(parts) > 1 else parts[0][1][None]
        got = lax.ppermute(sent, axis, xor_perm(size, bit))
        parts = parts + [(parts[i][0] ^ bit, got[i]) for i in range(len(parts))]
        bit //= 2
    return [p for _, p in sorted(parts, key=lambda item: item[0])]


def scatter_xor(partial, axis, size, rank):
    rows = partial.shape[0] // size
    held = partial.reshape(size, rows, -1)
    bit = 1
    while bit < size:
        view = held.reshape(held.shape[0] // 2, 2, rows, -1)
        mine = (rank // bit) % 2
        sent = pick(view, 1 - mine, 1).astype(jnp.bfloat16)
        got = lax.ppermute(sent, axis, xor_perm(size, bit))
        held = pick(view, mine, 1) + got.astype(jnp.float32)
        bit *= 2
    return held[0]


def ring_gather(chunk, axis, size, hold=None):
    order = ring_order(size)
    forward = [(order[i], order[(i + 1) % size]) for i in range(size)]
    backward = [(b, a) for a, b in forward]
    arrived = [(0, chunk)]
    ahead = behind = chunk
    for step in range(1, size // 2):
        ahead = lax.ppermute(ahead, axis, forward)
        behind = lax.ppermute(behind, axis, backward)
        arrived += [(step, ahead), (-step, behind)]
    half = chunk.shape[0] // 2
    top = lax.ppermute(ahead[:half], axis, forward)
    low = lax.ppermute(behind[half:], axis, backward)
    arrived.append((size // 2, jnp.concatenate([top, low], axis=0)))
    return arrived


def rope_tables(positions):
    half = ROPE // 2
    freqs = THETA ** (-jnp.arange(half, dtype=jnp.float32) / half)
    angle = positions[:, None] * freqs
    return jnp.cos(angle), jnp.sin(angle)


def one_head(query, normed, rotary, w_key, w_value, gain, nope, cosine, sine):
    depth = nope + ROPE
    head_nope = dot32(normed, w_key).astype(jnp.bfloat16).astype(jnp.float32)
    value = dot32(normed, w_value).astype(jnp.bfloat16)
    tail = rotary.astype(jnp.float32)
    squares = jnp.sum(head_nope * head_nope, -1, keepdims=True) + jnp.sum(tail * tail, -1, keepdims=True)
    scale = lax.rsqrt(squares / depth + EPSILON)
    head_nope = (head_nope * scale * gain[:nope]).astype(jnp.bfloat16)
    tail = tail * scale * gain[nope:]
    first, second = tail[:, : ROPE // 2], tail[:, ROPE // 2 :]
    turned = jnp.concatenate([first * cosine - second * sine, second * cosine + first * sine], axis=-1)
    key = jnp.concatenate([head_nope, turned.astype(jnp.bfloat16)], axis=-1)
    scores = lax.dot_general(query, key, (((1,), (1,)), ((), ())), preferred_element_type=jnp.float32)
    scores = scores * depth ** (-0.5)
    shifted = jnp.exp(scores - jnp.max(scores, axis=-1, keepdims=True))
    total = jnp.sum(shifted, axis=-1, keepdims=True)
    return (dot32(shifted.astype(jnp.bfloat16), value) / total).astype(jnp.bfloat16)


def heads_of(query, normed, rotary, w_key, w_value, gain, nope, cosine, sine):
    depth = nope + ROPE
    width = w_value.shape[1] * nope // w_key.shape[1]
    outs = []
    for h in range(w_key.shape[1] // nope):
        outs.append(
            one_head(
                query[:, h * depth : (h + 1) * depth],
                normed,
                rotary,
                w_key[:, h * nope : (h + 1) * nope],
                w_value[:, h * width : (h + 1) * width],
                gain,
                nope,
                cosine,
                sine,
            )
        )
    return jnp.concatenate(outs, axis=-1) if len(outs) > 1 else outs[0]


def make_body(sp, tp):
    order = ring_order(sp)
    place = [order.index(i) for i in range(sp)]
    direct = sp <= 16 and sp % 2 == 0

    def body(
        stream,
        query_a,
        query_b,
        latent,
        rotary_key,
        latent_gain,
        key_gain_a,
        key_gain_b,
        w_key_a,
        w_value_a,
        w_key_b,
        w_value_b,
        w_out_a,
        w_out_b,
        norm_gain,
        w_up,
        w_down,
    ):
        row = lax.axis_index("sp")
        rank = lax.axis_index("tp")
        core = rank % 2
        local = latent.shape[0]
        half = local // 2

        joined = jnp.concatenate([latent, rotary_key], axis=1)
        mine = lax.dynamic_slice_in_dim(joined, core * half, half, 0)
        steps = jnp.arange(sp, dtype=jnp.int32)
        if direct:
            pieces = [mine]
            for shift in range(1, sp):
                pieces.append(lax.ppermute(mine, "sp", [(i, (i + shift) % sp) for i in range(sp)]))
            near = jnp.concatenate(pieces, axis=0)
            starts = ((row - steps) % sp) * local
        else:
            near = lax.all_gather(mine, "sp", axis=0, tiled=True)
            starts = steps * local
        far = lax.ppermute(near, "tp", xor_perm(tp, 1))
        everything = jnp.concatenate([near, far], axis=0)
        inner = jnp.arange(half, dtype=jnp.int32)
        near_pos = (starts[:, None] + core * half + inner[None]).reshape(-1)
        far_pos = (starts[:, None] + (1 - core) * half + inner[None]).reshape(-1)
        cosine, sine = rope_tables(jnp.concatenate([near_pos, far_pos]).astype(jnp.float32))

        if direct:
            ups = ring_gather(w_up, "sp", sp)
            late, _ = lax.optimization_barrier((w_down, ups[3][1][:8]))
            downs = ring_gather(late, "sp", sp)
        else:
            up_full = lax.all_gather(w_up, "sp", axis=0, tiled=True)
            down_full = lax.all_gather(w_down, "sp", axis=1, tiled=True)

        outs = gather_xor(jnp.concatenate([w_out_a, w_out_b], axis=0), "tp", tp)
        streams = gather_xor(stream, "tp", tp)
        stacked = jnp.stack(streams)
        stream_all = jnp.concatenate([pick(stacked, rank ^ i, 0) for i in range(tp)], axis=0)

        channels = joined.shape[1] - ROPE
        rotary = everything[:, channels:]
        normed_latent = rms_scale(everything[:, :channels], latent_gain).astype(jnp.bfloat16)
        attended = jnp.concatenate(
            [
                heads_of(query_a, normed_latent, rotary, w_key_a, w_value_a, key_gain_a, NOPE_A, cosine, sine),
                heads_of(query_b, normed_latent, rotary, w_key_b, w_value_b, key_gain_b, NOPE_B, cosine, sine),
            ],
            axis=1,
        )
        attends = gather_xor(attended, "tp", tp)
        mixed = dot32(jnp.concatenate(attends, axis=1), jnp.concatenate(outs, axis=0))
        residual = (stream_all.astype(jnp.float32) + mixed).astype(jnp.bfloat16)
        normed = rms_scale(residual, norm_gain).astype(jnp.bfloat16)

        table = jnp.array(order, jnp.int32)
        position = jnp.array(place, jnp.int32)[row]

        def source(offset):
            return table[(position - offset) % sp]

        rows = stream.shape[0]
        own = lax.dynamic_slice_in_dim(residual, rank * rows, rows, 0).astype(jnp.float32)
        if not direct:
            activated = jnp.square(jax.nn.relu(dot32(normed, up_full))).astype(jnp.bfloat16)
            return (own + scatter_xor(dot32(activated, down_full), "tp", tp, rank)).astype(jnp.bfloat16)

        width = w_up.shape[0]
        hidden = 0.0
        for offset, chunk in ups:
            hidden = hidden + dot32(lax.dynamic_slice_in_dim(normed, source(offset) * width, width, 1), chunk)
        activated = jnp.square(jax.nn.relu(hidden)).astype(jnp.bfloat16)

        columns = w_down.shape[1]
        result = jnp.zeros(stream.shape, jnp.bfloat16)
        groups = [downs[:3], downs[3:5], downs[5:7], downs[7:]] if len(downs) == 8 else [[d] for d in downs]
        for group in groups:
            weights = jnp.concatenate([c for _, c in group], axis=1) if len(group) > 1 else group[0][1]
            summed = scatter_xor(dot32(activated, weights), "tp", tp, rank)
            for i, (offset, _) in enumerate(group):
                start = source(offset) * columns
                block = lax.dynamic_slice_in_dim(own, start, columns, 1) + summed[:, i * columns : (i + 1) * columns]
                result = lax.dynamic_update_slice_in_dim(result, block.astype(jnp.bfloat16), start, 1)
        return result

    return body


def solution(mesh):
    in_specs = (
        P(("sp", "tp"), None),
        P("sp", "tp"),
        P("sp", "tp"),
        P("sp", None),
        P("sp", None),
        P(),
        P(),
        P(),
        P(None, "tp"),
        P(None, "tp"),
        P(None, "tp"),
        P(None, "tp"),
        P("tp", None),
        P("tp", None),
        P(),
        P("sp", "tp"),
        P("tp", "sp"),
    )
    out_specs = P(("sp", "tp"), None)
    body = make_body(mesh.shape["sp"], mesh.shape["tp"])
    return jax.shard_map(body, mesh=mesh, in_specs=in_specs, out_specs=out_specs, check_vma=False)
```

```python
import jax
import jax.numpy as jnp
from jax import lax
from jax.sharding import PartitionSpec as P

NOPE_A = 64
V_A = 64
NOPE_B = 128
V_B = 128
ROPE = 32


EPSILON = 1e-06
THETA = 10000.0


def rms_scale(values, gain):
    wide = values.astype(jnp.float32)
    return wide * lax.rsqrt(jnp.mean(wide * wide, axis=-1, keepdims=True) + EPSILON) * gain


def dot32(a, b):
    return jnp.dot(a, b, preferred_element_type=jnp.float32)


def pick(array, index, axis):
    return jnp.squeeze(slice_at(array, index, 1, axis), axis)


def slice_at(array, start, size, axis):
    starts = [jnp.zeros((), jnp.int32)] * array.ndim
    starts[axis] = start
    sizes = list(array.shape)
    sizes[axis] = size
    return lax.dynamic_slice(array, starts, sizes, allow_negative_indices=False)


def place_at(array, block, start, axis):
    starts = [jnp.zeros((), jnp.int32)] * array.ndim
    starts[axis] = start
    return lax.dynamic_update_slice(array, block, starts, allow_negative_indices=False)


def xor_perm(size, bit):
    return [(i, i ^ bit) for i in range(size)]


def ring_order(size):
    return list(range(0, size, 2)) + list(range(size - 1, 0, -2))


def gather_xor(block, axis, size):
    parts = [(0, block)]
    bit = size // 2
    while bit:
        sent = jnp.stack([p for _, p in parts]) if len(parts) > 1 else parts[0][1][None]
        got = lax.ppermute(sent, axis, xor_perm(size, bit))
        parts = parts + [(parts[i][0] ^ bit, got[i]) for i in range(len(parts))]
        bit //= 2
    return [p for _, p in sorted(parts, key=lambda item: item[0])]


def scatter_xor(partial, axis, size, rank):
    rows = partial.shape[0] // size
    held = partial.reshape(size, rows, -1)
    bit = 1
    while bit < size:
        view = held.reshape(held.shape[0] // 2, 2, rows, -1)
        mine = (rank & bit) // bit
        sent = pick(view, 1 - mine, 1).astype(jnp.bfloat16)
        got = lax.ppermute(sent, axis, xor_perm(size, bit))
        held = pick(view, mine, 1) + got.astype(jnp.float32)
        bit *= 2
    return held[0]


def ring_gather(chunk, axis, size, hold=None):
    order = ring_order(size)
    forward = [(order[i], order[(i + 1) % size]) for i in range(size)]
    backward = [(b, a) for a, b in forward]
    arrived = [(0, chunk)]
    ahead = behind = chunk
    for step in range(1, size // 2):
        ahead = lax.ppermute(ahead, axis, forward)
        behind = lax.ppermute(behind, axis, backward)
        arrived += [(step, ahead), (-step, behind)]
    half = chunk.shape[0] // 2
    top = lax.ppermute(ahead[:half], axis, forward)
    low = lax.ppermute(behind[half:], axis, backward)
    arrived.append((size // 2, jnp.concatenate([top, low], axis=0)))
    return arrived


def rope_tables(positions):
    half = ROPE // 2
    freqs = THETA ** (-jnp.arange(half, dtype=jnp.float32) / half)
    angle = positions[:, None] * freqs
    return jnp.cos(angle), jnp.sin(angle)


def one_head(query, normed, rotary, w_key, w_value, gain, nope, cosine, sine):
    depth = nope + ROPE
    head_nope = dot32(normed, w_key).astype(jnp.bfloat16).astype(jnp.float32)
    value = dot32(normed, w_value).astype(jnp.bfloat16)
    tail = rotary.astype(jnp.float32)
    squares = jnp.sum(head_nope * head_nope, -1, keepdims=True) + jnp.sum(tail * tail, -1, keepdims=True)
    scale = lax.rsqrt(squares / depth + EPSILON)
    head_nope = (head_nope * scale * gain[:nope]).astype(jnp.bfloat16)
    tail = tail * scale * gain[nope:]
    first, second = tail[:, : ROPE // 2], tail[:, ROPE // 2 :]
    turned = jnp.concatenate([first * cosine - second * sine, second * cosine + first * sine], axis=-1)
    key = jnp.concatenate([head_nope, turned.astype(jnp.bfloat16)], axis=-1)
    scores = lax.dot_general(query, key, (((1,), (1,)), ((), ())), preferred_element_type=jnp.float32)
    scores = scores * depth ** (-0.5)
    shifted = jnp.exp(scores - jnp.max(scores, axis=-1, keepdims=True))
    total = jnp.sum(shifted, axis=-1, keepdims=True)
    return (dot32(shifted.astype(jnp.bfloat16), value) / total).astype(jnp.bfloat16)


def heads_of(query, normed, rotary, w_key, w_value, gain, nope, cosine, sine):
    depth = nope + ROPE
    width = w_value.shape[1] * nope // w_key.shape[1]
    outs = []
    for h in range(w_key.shape[1] // nope):
        outs.append(
            one_head(
                query[:, h * depth : (h + 1) * depth],
                normed,
                rotary,
                w_key[:, h * nope : (h + 1) * nope],
                w_value[:, h * width : (h + 1) * width],
                gain,
                nope,
                cosine,
                sine,
            )
        )
    return jnp.concatenate(outs, axis=-1) if len(outs) > 1 else outs[0]


def make_body(sp, tp):
    order = ring_order(sp)
    place = [order.index(i) for i in range(sp)]
    direct = sp <= 16 and sp % 2 == 0

    def body(
        stream,
        query_a,
        query_b,
        latent,
        rotary_key,
        latent_gain,
        key_gain_a,
        key_gain_b,
        w_key_a,
        w_value_a,
        w_key_b,
        w_value_b,
        w_out_a,
        w_out_b,
        norm_gain,
        w_up,
        w_down,
    ):
        row = lax.axis_index("sp")
        rank = lax.axis_index("tp")
        core = rank & 1
        local = latent.shape[0]
        half = local // 2

        joined = jnp.concatenate([latent, rotary_key], axis=1)
        mine = slice_at(joined, core * half, half, 0)
        steps = jnp.arange(sp, dtype=jnp.int32)
        if direct:
            pieces = [mine]
            for shift in range(1, sp):
                pieces.append(lax.ppermute(mine, "sp", [(i, (i + shift) % sp) for i in range(sp)]))
            near = jnp.concatenate(pieces, axis=0)
            starts = ((row + sp - steps) % sp) * local
        else:
            near = lax.all_gather(mine, "sp", axis=0, tiled=True)
            starts = steps * local
        far = lax.ppermute(near, "tp", xor_perm(tp, 1))
        everything = jnp.concatenate([near, far], axis=0)
        inner = jnp.arange(half, dtype=jnp.int32)
        near_pos = (starts[:, None] + core * half + inner[None]).reshape(-1)
        far_pos = (starts[:, None] + (1 - core) * half + inner[None]).reshape(-1)
        cosine, sine = rope_tables(jnp.concatenate([near_pos, far_pos]).astype(jnp.float32))

        if direct:
            ups = ring_gather(w_up, "sp", sp)
            late, _ = lax.optimization_barrier((w_down, ups[3][1][:8]))
            downs = ring_gather(late, "sp", sp)
        else:
            up_full = lax.all_gather(w_up, "sp", axis=0, tiled=True)
            down_full = lax.all_gather(w_down, "sp", axis=1, tiled=True)

        outs = gather_xor(jnp.concatenate([w_out_a, w_out_b], axis=0), "tp", tp)
        streams = gather_xor(stream, "tp", tp)
        stacked = jnp.stack(streams)
        stream_all = jnp.concatenate([pick(stacked, rank ^ i, 0) for i in range(tp)], axis=0)

        channels = joined.shape[1] - ROPE
        rotary = everything[:, channels:]
        normed_latent = rms_scale(everything[:, :channels], latent_gain).astype(jnp.bfloat16)
        attended = jnp.concatenate(
            [
                heads_of(query_a, normed_latent, rotary, w_key_a, w_value_a, key_gain_a, NOPE_A, cosine, sine),
                heads_of(query_b, normed_latent, rotary, w_key_b, w_value_b, key_gain_b, NOPE_B, cosine, sine),
            ],
            axis=1,
        )
        attends = gather_xor(attended, "tp", tp)
        mixed = dot32(jnp.concatenate(attends, axis=1), jnp.concatenate(outs, axis=0))
        residual = (stream_all.astype(jnp.float32) + mixed).astype(jnp.bfloat16)
        normed = rms_scale(residual, norm_gain).astype(jnp.bfloat16)

        position = jnp.where(row & 1, sp - 1 - (row >> 1), row >> 1)
        found = {}

        def source(offset):
            if offset not in found:
                spot = position - offset
                spot = jnp.where(spot < 0, spot + sp, spot) if offset > 0 else spot
                spot = jnp.where(spot >= sp, spot - sp, spot) if offset < 0 else spot
                found[offset] = jnp.minimum(2 * spot, 2 * sp - 1 - 2 * spot)
            return found[offset]

        rows = stream.shape[0]
        own = slice_at(residual, rank * rows, rows, 0).astype(jnp.float32)
        if not direct:
            activated = jnp.square(jax.nn.relu(dot32(normed, up_full))).astype(jnp.bfloat16)
            return (own + scatter_xor(dot32(activated, down_full), "tp", tp, rank)).astype(jnp.bfloat16)

        width = w_up.shape[0]
        hidden = 0.0
        for offset, chunk in ups:
            hidden = hidden + dot32(slice_at(normed, source(offset) * width, width, 1), chunk)
        activated = jnp.square(jax.nn.relu(hidden)).astype(jnp.bfloat16)

        columns = w_down.shape[1]
        result = jnp.zeros(stream.shape, jnp.bfloat16)
        groups = [downs[:3], downs[3:5], downs[5:7], downs[7:]] if len(downs) == 8 else [[d] for d in downs]
        for group in groups:
            weights = jnp.concatenate([c for _, c in group], axis=1) if len(group) > 1 else group[0][1]
            summed = scatter_xor(dot32(activated, weights), "tp", tp, rank)
            for i, (offset, _) in enumerate(group):
                start = source(offset) * columns
                block = slice_at(own, start, columns, 1) + summed[:, i * columns : (i + 1) * columns]
                result = place_at(result, block.astype(jnp.bfloat16), start, 1)
        return result

    return body


def solution(mesh):
    in_specs = (
        P(("sp", "tp"), None),
        P("sp", "tp"),
        P("sp", "tp"),
        P("sp", None),
        P("sp", None),
        P(),
        P(),
        P(),
        P(None, "tp"),
        P(None, "tp"),
        P(None, "tp"),
        P(None, "tp"),
        P("tp", None),
        P("tp", None),
        P(),
        P("sp", "tp"),
        P("tp", "sp"),
    )
    out_specs = P(("sp", "tp"), None)
    body = make_body(mesh.shape["sp"], mesh.shape["tp"])
    return jax.shard_map(body, mesh=mesh, in_specs=in_specs, out_specs=out_specs, check_vma=False)
```
